32 devices in a mesh: fs: 16 (over z, y, core), tp: 2 (over x).
Axes of the slice: x: 2, y: 2, z: 4, core: 2. Of those that a mesh axis runs over, the one named last changes fastest.
Arguments:
- inputs: bfloat16 [16384, 3072], P('fs'), may hold values from -6 to 6
- query_cot: bfloat16 [16384, 768], P('fs', 'tp'), may hold values from -0.046875 to 0.046875
- value_cot: bfloat16 [16384, 1536], P('fs', 'tp'), may hold values from -0.046875 to 0.046875
- query_factor: bfloat16 [3072, 192], P('fs'), may hold values from -0.109375 to 0.109375
- value_factor: bfloat16 [3072, 192], P('fs'), may hold values from -0.109375 to 0.109375
- query_weight: float32 [3072, 768], P('fs', 'tp'), may hold values from -0.109375 to 0.109375
- value_weight: float32 [3072, 1536], P('fs', 'tp'), may hold values from -0.109375 to 0.109375
- query_first: float32 [192, 768], P('fs', 'tp'), may hold values from -1.6 to 1.6
- query_second: float32 [192, 768], P('fs', 'tp'), may hold values from 0.002 to 0.05
- value_first: float32 [192, 1536], P('fs', 'tp'), may hold values from -1.6 to 1.6
- value_second: float32 [192, 1536], P('fs', 'tp'), may hold values from 0.002 to 0.05
Outputs:
- step_q: float32 [3072, 768], P('fs', 'tp')
- step_v: float32 [3072, 1536], P('fs', 'tp')
- new_q: float32 [3072, 768], P('fs', 'tp')
- new_v: float32 [3072, 1536], P('fs', 'tp')
- first_q: float32 [192, 768], P('fs', 'tp')
- second_q: float32 [192, 768], P('fs', 'tp')
- first_v: float32 [192, 1536], P('fs', 'tp')
- second_v: float32 [192, 1536], P('fs', 'tp')
- copy_q: bfloat16 [3072, 768], P(None, 'tp')
- copy_v: bfloat16 [3072, 1536], P(None, 'tp')
The draws below stay inside these ranges and needn't reach their ends.
All inputs are finite; a program needn't handle non-finite values.
Results may differ from the reference program's by a relative error of at most 0.0041.
Values may be sent and summed in bfloat16 or wider, within the bound.
A program may use at most 64 MiB of HBM per device.

```python
import math
import jax
import jax.numpy as jnp
from jax import lax

D = 3072
QW = 768
VW = 1536
R = 192
TOKENS = 16384


def draw_query_first(key, part):
    ramp = 1.0 + 3.0 * jnp.arange(R, dtype=jnp.float32)[:, None] / (R - 1)
    noise = jnp.clip(jax.random.normal(key, (R, QW), jnp.float32), -4.0, 4.0)
    return 0.1 * ramp * noise


def draw_value_first(key, part):
    ramp = 1.0 + 3.0 * jnp.arange(R, dtype=jnp.float32)[:, None] / (R - 1)
    noise = jnp.clip(jax.random.normal(key, (R, VW), jnp.float32), -4.0, 4.0)
    return 0.1 * ramp * noise


def steps_of(stream_key, dims, split, least, largest):
    gain = 1.0
    for axis_at, blocks in split:
        heights = jax.random.uniform(jax.random.fold_in(jax.random.fold_in(stream_key, 6), axis_at), (blocks,), jnp.float32, least / len(split), largest / len(split))
        gain = gain * jnp.repeat(jnp.exp(heights), dims[axis_at] // blocks).reshape((-1,) + (1,) * (len(dims) - 1 - axis_at))
    return gain


def centred(own_key, extent, width, bound, shards=(), kind=jnp.bfloat16):
    factor_of = steps_of(own_key, extent, shards, -0.22, 0.18) if shards else 1.0
    array = jax.random.normal(own_key, extent, jnp.float32) * width * factor_of
    return jnp.minimum(jnp.maximum(array, -bound), bound).astype(kind)


def setup_inputs(seed: int = 0) -> dict:
    streams_of = jax.random.split(jax.random.key(seed), 12)
    return {
        "inputs": centred(streams_of[0], (TOKENS, D), 1.0, 6.0, ((0, 16),)),
        "query_cot": centred(streams_of[1], (TOKENS, QW), (TOKENS ** -0.5), 0.046875, ((0, 16), (1, 2))),
        "value_cot": centred(streams_of[2], (TOKENS, VW), (TOKENS ** -0.5), 0.046875, ((0, 16), (1, 2))),
        "query_factor": centred(streams_of[3], (D, R), D ** -0.5, 0.109375, ((0, 16),)),
        "value_factor": centred(streams_of[4], (D, R), D ** -0.5, 0.109375, ((0, 16),)),
        "query_weight": centred(streams_of[5], (D, QW), D ** -0.5, 0.109375, ((0, 16), (1, 2)), jnp.float32),
        "value_weight": centred(streams_of[6], (D, VW), D ** -0.5, 0.109375, ((0, 16), (1, 2)), jnp.float32),
        "query_first": draw_query_first(jax.random.fold_in(streams_of[11], 71), 0),
        "query_second": jnp.clip(jnp.exp(math.log(0.05) - 3.218876 * jax.random.uniform(streams_of[8], (R, QW), jnp.float32) ** steps_of(streams_of[8], (R, QW), ((0, 16), (1, 2)), -0.2, 0.2)), 0.002, 0.05),
        "value_first": draw_value_first(jax.random.fold_in(streams_of[11], 71), 0),
        "value_second": jnp.clip(jnp.exp(math.log(0.05) - 3.218876 * jax.random.uniform(streams_of[10], (R, VW), jnp.float32) ** steps_of(streams_of[10], (R, VW), ((0, 16), (1, 2)), -0.2, 0.2)), 0.002, 0.05),
    }


first_decay = 0.9
second_decay = 0.99
small_eps = 1e-08
learn_rate = 0.01

def moments(old_first, old_second, gradient):
    first = first_decay * old_first + (1.0 - first_decay) * gradient
    second = second_decay * old_second + (1.0 - second_decay) * gradient * gradient
    unit = first / (jnp.sqrt(second) + small_eps)
    return (first, second, unit)

def reference(inputs, query_cot, value_cot, query_factor, value_factor, query_weight, value_weight, query_first, query_second, value_first, value_second):
    proj_q = jnp.dot(inputs, query_factor, preferred_element_type=jnp.float32).astype(jnp.bfloat16)
    proj_v = jnp.dot(inputs, value_factor, preferred_element_type=jnp.float32).astype(jnp.bfloat16)
    grad_q = jnp.dot(proj_q.T, query_cot, preferred_element_type=jnp.float32)
    grad_v = jnp.dot(proj_v.T, value_cot, preferred_element_type=jnp.float32)
    first_q, second_q, unit_q = moments(query_first, query_second, grad_q)
    first_v, second_v, unit_v = moments(value_first, value_second, grad_v)
    entries = float(unit_q.size + unit_v.size)
    step_scale = lax.rsqrt((jnp.sum(unit_q * unit_q) + jnp.sum(unit_v * unit_v)) / entries + 1e-06)
    bits_q = (step_scale * unit_q).astype(jnp.bfloat16)
    bits_v = (step_scale * unit_v).astype(jnp.bfloat16)
    step_q = jnp.dot(query_factor, bits_q, preferred_element_type=jnp.float32)
    step_v = jnp.dot(value_factor, bits_v, preferred_element_type=jnp.float32)
    new_q = query_weight - learn_rate * step_q
    new_v = value_weight - learn_rate * step_v
    return (step_q, step_v, new_q, new_v, first_q, second_q, first_v, second_v, new_q.astype(jnp.bfloat16), new_v.astype(jnp.bfloat16))
```

```python
import functools

import jax
import jax.numpy as jnp
from jax import lax
from jax.experimental import pallas as pl
from jax.experimental.pallas import tpu as pltpu
from jax.sharding import PartitionSpec as P

first_decay = 0.9
second_decay = 0.99
small_eps = 1e-08
learn_rate = 0.01
CORES = 2
COLS = 2
TPS = 2
HALVES = 2
DEPTH = 4
WIRE = jnp.bfloat16


def moments(old_first, old_second, gradient):
    first = first_decay * old_first + (1.0 - first_decay) * gradient
    second = second_decay * old_second + (1.0 - second_decay) * gradient * gradient
    unit = first / (jnp.sqrt(second) + small_eps)
    return (first, second, unit)


class Place:
    def __init__(self, n):
        self.depth = n // (COLS * CORES)
        self.me = lax.axis_index("fs")
        self.tp = lax.axis_index("tp")
        self.c = self.me % CORES
        self.y = (self.me // CORES) % COLS
        self.z = self.me // (CORES * COLS)

    def at(self, z, y, c):
        return (z * COLS + y) * CORES + c

    def near(self, i):
        if i == 0:
            return self.z
        below, above = self.z, self.depth - 1 - self.z
        both = jnp.minimum(below, above)
        turn = self.z - (i + 1) // 2 if i % 2 else self.z + i // 2
        far = jnp.where(below < above, self.z + (i - both), self.z - (i - both))
        return jnp.where(i <= 2 * both, turn, far)

    def col(self, j):
        return self.y if j == 0 else 1 - self.y

    def to_z(self, z):
        return {"fs": self.at(z, self.y, self.c)}

    def to_y(self):
        return {"fs": self.at(self.z, 1 - self.y, self.c)}

    def to_c(self):
        return {"fs": self.at(self.z, self.y, 1 - self.c)}

    def to_x(self):
        return {"tp": 1 - self.tp}


class Mail:
    def __init__(self, place):
        self.p = place
        self.sent = []

    def send(self, src, dst, ss, rs, peer, when=None):
        def make():
            return pltpu.make_async_remote_copy(
                src_ref=src, dst_ref=dst, send_sem=ss, recv_sem=rs,
                device_id=peer, device_id_type=pl.DeviceIdType.MESH)

        if when is None:
            make().start()
        else:
            pl.when(when)(lambda: make().start())
        self.sent.append((when, make))

    def got(self, dst, ss, rs):
        pltpu.make_async_remote_copy(
            src_ref=dst, dst_ref=dst, send_sem=ss, recv_sem=rs,
            device_id=self.p.to_c(), device_id_type=pl.DeviceIdType.MESH).wait_recv()

    def drain(self):
        for when, make in self.sent:
            if when is None:
                make().wait_send()
            else:
                pl.when(when)(lambda make=make: make().wait_send())


class Factors:
    def __init__(self, place, mail, full, spread, sems):
        self.p, self.m, self.full = place, mail, full
        self.zs, self.zr, self.ys, self.yr, self.xs, self.xr, self.cs, self.cr = sems
        rows = full.shape[1]
        rest = rows - spread
        self.mine = pl.ds(pl.multiple_of(place.tp * rest, 16), spread)
        self.give = pl.ds(pl.multiple_of(place.tp * spread, 16), rest)
        self.take = pl.ds(pl.multiple_of((1 - place.tp) * spread, 16), rest)

    def view(self, j, i, rows, c=None):
        p = self.p
        return self.full.at[p.at(p.near(i), p.col(j), p.c if c is None else c), rows]

    def own(self):
        p, v = self.p, self.view(0, 0, self.mine)
        for i in range(1, p.depth):
            self.m.send(v, v, self.zs.at[i], self.zr.at[p.z], p.to_z(p.near(i)))
        self.m.send(v, v, self.ys.at[0], self.yr.at[p.z], p.to_y())
        whole = self.full.at[p.me]
        self.m.send(whole, whole, self.cs.at[0, 0, 0], self.cr.at[0, 0, p.z], p.to_c())

    def pass_xc(self, j, i):
        p = self.p
        z = p.near(i)
        v, g = self.view(j, i, self.mine), self.view(j, i, self.give)
        self.m.send(g, g, self.xs.at[j, i], self.xr.at[j, z], p.to_x())
        self.m.send(v, v, self.cs.at[0, j, i], self.cr.at[0, j, z], p.to_c())

    def z(self, i):
        p = self.p
        v = self.view(0, i, self.mine)
        self.m.got(v, self.zs.at[i], self.zr.at[p.near(i)])
        self.m.send(v, v, self.ys.at[i], self.yr.at[p.near(i)], p.to_y())
        self.pass_xc(0, i)

    def y(self, i):
        v = self.view(1, i, self.mine)
        self.m.got(v, self.ys.at[i], self.yr.at[self.p.near(i)])
        self.pass_xc(1, i)

    def x(self, j, i):
        p = self.p
        z = p.near(i)
        v = self.view(j, i, self.take)
        self.m.got(v, self.xs.at[j, i], self.xr.at[j, z])
        self.m.send(v, v, self.cs.at[1, j, i], self.cr.at[1, j, z], p.to_c())

    def core(self, j, i):
        p = self.p
        z = p.near(i)
        if j == 0 and i == 0:
            self.m.got(self.full.at[p.at(z, p.y, 1 - p.c)], self.cs.at[0, 0, 0], self.cr.at[0, 0, z])
            return
        self.m.got(self.view(j, i, self.mine, 1 - p.c), self.cs.at[0, j, i], self.cr.at[0, j, z])
        self.m.got(self.view(j, i, self.take, 1 - p.c), self.cs.at[1, j, i], self.cr.at[1, j, z])


class Weights:
    def __init__(self, place, mail, full, sems):
        self.p, self.m, self.full = place, mail, full
        self.zs, self.es, self.zr, self.ys, self.yr, self.cs, self.cr = sems
        self.half = full.shape[1] // HALVES

    def view(self, j, i, h, c=None):
        p = self.p
        slot = p.at(p.near(i), p.col(j), p.c if c is None else c)
        return self.full.at[slot, pl.ds(h * self.half, self.half)]

    def own_z(self, h):
        p, v = self.p, self.view(0, 0, h)
        for d, to in ((0, p.z + 1), (1, p.z - 1)):
            ok = to < p.depth if d == 0 else to >= 0
            self.m.send(v, v, self.zs.at[d, 0, h], self.zr.at[p.z, h], p.to_z(to), ok)

    def to_core(self, j, i, h):
        p, v = self.p, self.view(j, i, h)
        self.m.send(v, v, self.cs.at[j, i, h], self.cr.at[j, p.near(i), h], p.to_c())

    def own_y(self, h):
        p, v = self.p, self.view(0, 0, h)
        self.m.send(v, v, self.ys.at[0, h], self.yr.at[p.z, h], p.to_y())

    def z(self, i, h):
        p, v = self.p, self.view(0, i, h)
        frm = p.near(i)
        self.m.got(v, self.zs.at[0, i, h], self.zr.at[frm, h])
        to = jnp.where(frm < p.z, p.z + 1, p.z - 1)
        ok = jnp.logical_and(to >= 0, to < p.depth)
        self.m.send(v, v, self.zs.at[0, i, h], self.zr.at[frm, h], p.to_z(to), ok)
        if h > 0 or i > 2:
            when = None
        else:
            when = jnp.logical_and(frm != p.z + 1, frm != p.z - 1)
        if not (h == 0 and i == 1):
            self.m.send(v, v, self.ys.at[i, h], self.yr.at[frm, h], p.to_y(), when)
        self.to_core(0, i, h)

    def y(self, i, h):
        p, v = self.p, self.view(1, i, h)
        self.m.got(v, self.ys.at[i, h], self.yr.at[p.near(i), h])
        if i == 0 and h == 0:
            for d, to in ((0, p.z + 1), (1, p.z - 1)):
                ok = to < p.depth if d == 0 else to >= 0
                self.m.send(v, v, self.es.at[d], self.yr.at[p.z, h], p.to_z(to), ok)
        self.to_core(1, i, h)

    def core(self, j, i):
        p = self.p
        for h in range(HALVES):
            self.m.got(self.view(j, i, h, 1 - p.c), self.cs.at[j, i, h], self.cr.at[j, p.near(i), h])


class Units:
    def __init__(self, place, mail, full, sems):
        self.p, self.m, self.full = place, mail, full
        self.zs, self.zr, self.ys, self.yr, self.cs, self.cr = sems

    def view(self, j, i, c=None):
        p = self.p
        return self.full.at[p.at(p.near(i), p.col(j), p.c if c is None else c)]

    def to_core(self, j, i):
        p, v = self.p, self.view(j, i)
        self.m.send(v, v, self.cs.at[j, i], self.cr.at[j, p.near(i)], p.to_c())

    def to_col(self, i):
        p, v = self.p, self.view(0, i)
        self.m.send(v, v, self.ys.at[i], self.yr.at[p.near(i)], p.to_y())

    def own(self):
        p, v = self.p, self.view(0, 0)
        for i in range(p.depth - 1, 0, -1):
            self.m.send(v, v, self.zs.at[i], self.zr.at[p.z], p.to_z(p.near(i)))
        self.to_col(0)
        self.to_core(0, 0)

    def z(self, i):
        self.m.got(self.view(0, i), self.zs.at[i], self.zr.at[self.p.near(i)])
        self.to_col(i)
        self.to_core(0, i)

    def y(self, i):
        self.m.got(self.view(1, i), self.ys.at[i], self.yr.at[self.p.near(i)])
        self.to_core(1, i)

    def core(self, j, i):
        p = self.p
        self.m.got(self.view(j, i, 1 - p.c), self.cs.at[j, i], self.cr.at[j, p.near(i)])


def semaphores(depth):
    dma = pltpu.SemaphoreType.DMA
    line = [dma((depth,))]
    factors = line * 4 + [dma((COLS, depth))] * 2 + [dma((2, COLS, depth))] * 2
    weights = [
        dma((2, depth, HALVES)), dma((2,)), dma((depth, HALVES)), dma((depth, HALVES)), dma((depth, HALVES)),
        dma((COLS, depth, HALVES)), dma((COLS, depth, HALVES))]
    units = line * 4 + [dma((COLS, depth))] * 2
    return factors, weights, units


def kernel(
    n, counts, x_hbm, cq_hbm, cv_hbm, qf_hbm, vf_hbm, qw_hbm, vw_hbm, q1_hbm, q2_hbm, v1_hbm, v2_hbm,
    step_q, step_v, new_q, new_v, first_q, second_q, first_v, second_v, copy_q, copy_v,
    x, cq, cv, qf, vf, qw, vw, q1, q2, v1, v2,
    f_all, w_all, u_all, g, g_core, g_send, g_col, g_line, g_deep, g_part, u_flat, u_half, sq, sq_in,
    acc_q, acc_v, local, gcs, gzs, gzr, tsem, *sems):
    p = Place(n)
    depth = p.depth
    rows = q1.shape[0]
    rank, q_cols = acc_q.shape
    deep = w_all.shape[1]
    m = Mail(p)
    n_f, n_w, _ = counts
    F = Factors(p, m, f_all, deep // 2, sems[:n_f])
    W = Weights(p, m, w_all, sems[n_f:n_f + n_w])
    U = Units(p, m, u_all, sems[n_f + n_w:])
    others = range(1, depth)
    pairs = (
        (qf_hbm, qf), (vf_hbm, vf), (qw_hbm, qw), (vw_hbm, vw), (x_hbm, x), (cq_hbm, cq), (cv_hbm, cv),
        (q1_hbm, q1), (q2_hbm, q2), (v1_hbm, v1), (v2_hbm, v2))
    loads = [pltpu.make_async_copy(src, dst, local.at[i]) for i, (src, dst) in enumerate(pairs)]
    for copy in loads:
        copy.start()

    scope = jax.named_scope
    barrier = pltpu.get_barrier_semaphore()
    peers = [p.to_z(p.near(i)) for i in others] + [p.to_y(), p.to_c(), p.to_x()]
    with scope("enter"):
        for peer in peers:
            pl.semaphore_signal(barrier, inc=1, device_id=peer, device_id_type=pl.DeviceIdType.MESH)
        loads[0].wait()
        loads[1].wait()
        f_all[p.me, :, :rank] = qf[...]
        f_all[p.me, :, rank:] = vf[...]
    with scope("barrier"):
        pl.semaphore_wait(barrier, len(peers))
    F.own()
    with scope("load_w"):
        loads[2].wait()
        loads[3].wait()
        w_all[p.me, :, :q_cols] = qw[...].astype(jnp.bfloat16)
        w_all[p.me, :, q_cols:] = vw[...].astype(jnp.bfloat16)
    for h in range(HALVES):
        W.own_z(h)
    for i in others:
        with scope(f"fz{i}"):
            F.z(i)
    for h in range(HALVES):
        W.own_y(h)
        W.to_core(0, 0, h)
    for i in range(depth):
        with scope(f"fy{i}"):
            F.y(i)
    for i in others:
        with scope(f"fx0{i}"):
            F.x(0, i)
    for i in range(depth):
        with scope(f"fx1{i}"):
            F.x(1, i)
    with scope("fc"):
        for j in range(COLS):
            for i in range(depth):
                F.core(j, i)
    with scope("wz10"):
        W.z(1, 0)
    with scope("wz20"):
        W.z(2, 0)
    with scope("wy00"):
        W.y(0, 0)
    with scope("loads"):
        for copy in loads[4:]:
            copy.wait()

    tile = 256
    with scope("mm"):
        acc_q[...] = jnp.zeros_like(acc_q)
        acc_v[...] = jnp.zeros_like(acc_v)

        @pl.loop(0, x.shape[0] // tile)
        def _(k):
            at = pl.ds(pl.multiple_of(k * tile, tile), tile)
            f = f_all[...].reshape(x.shape[1], 2 * rank)
            proj = jnp.dot(x[at, :], f, preferred_element_type=jnp.float32)
            turned = proj.T.astype(jnp.bfloat16)
            acc_q[...] += jnp.dot(turned[:rank], cq[at, :], preferred_element_type=jnp.float32)
            acc_v[...] += jnp.dot(turned[rank:], cv[at, :], preferred_element_type=jnp.float32)

    with scope("gstore"):
        for j in range(n):
            c, y, z = j % CORES, (j // CORES) % COLS, j // (CORES * COLS)
            at = slice(z * rows, (z + 1) * rows)
            g[c, y, at, :q_cols] = acc_q[j * rows:(j + 1) * rows, :]
            g[c, y, at, q_cols:] = acc_v[j * rows:(j + 1) * rows, :]

    other = g.at[1 - p.c]
    m.send(other, g_core, gcs.at[0], gcs.at[1], p.to_c())
    with scope("wz11"):
        W.z(1, 1)
    with scope("wz21"):
        W.z(2, 1)
    with scope("wy01"):
        W.y(0, 1)
    with scope("gcore"):
        m.got(g_core, gcs.at[0], gcs.at[1])
        g_send[...] = (g[p.c, 1 - p.y] + g_core[1 - p.y]).astype(g_send.dtype)
    m.send(g_send, g_col, gcs.at[2], gcs.at[3], p.to_y())
    with scope("wy10"):
        W.y(1, 0)
    with scope("wz30"):
        W.z(3, 0)
    with scope("gcol"):
        m.got(g_col, gcs.at[2], gcs.at[3])
        mine = g[p.c, p.y] + g_core[p.y] + g_col[...].astype(jnp.float32)
        for z in range(depth):
            part = mine[z * rows:(z + 1) * rows]
            g_part[z] = part
            g_line[z] = part.astype(g_line.dtype)
    for i in range(depth - 1, 0, -1):
        to = p.near(i)
        m.send(g_line.at[to], g_deep.at[p.z], gzs.at[i], gzr.at[p.z], p.to_z(to))
    with scope("wy11"):
        W.y(1, 1)
    with scope("gline"):
        total = g_part[p.z]
        for i in others:
            frm = p.near(i)
            m.got(g_deep.at[frm], gzs.at[i], gzr.at[frm])
            total = total + g_deep[frm].astype(jnp.float32)
    with scope("moments"):
        first, second, unit = moments(q1[...], q2[...], total[:, :q_cols])
        first_q[...], second_q[...] = first, second
        u_all[p.me, :, :q_cols] = unit.astype(u_all.dtype)
        first, second, unit = moments(v1[...], v2[...], total[:, q_cols:])
        first_v[...], second_v[...] = first, second
        u_all[p.me, :, q_cols:] = unit.astype(u_all.dtype)
    U.own()
    for i in others:
        with scope(f"uz{i}"):
            U.z(i)
    for i in range(depth):
        with scope(f"uy{i}"):
            U.y(i)
    with scope("uc"):
        for j in range(COLS):
            for i in range(depth):
                U.core(j, i)
    with scope("norm"):
        for j in range(n):
            u_flat[j * rows:(j + 1) * rows, :] = u_all[j].astype(jnp.float32)
        whole = u_flat[...]
        u_half[...] = whole.astype(jnp.bfloat16)
        sq[...] = jnp.full(sq.shape, jnp.sum(whole * whole), jnp.float32)
        m.send(sq, sq_in, tsem.at[0], tsem.at[1], p.to_x())
    with scope("wz31"):
        W.z(3, 1)
    for i in range(2, depth):
        for h in range(HALVES):
            with scope(f"wy{i}{h}"):
                W.y(i, h)
    with scope("sq"):
        m.got(sq_in, tsem.at[0], tsem.at[1])
        entries = rank * (q_cols + acc_v.shape[1]) * TPS
        scale = lax.rsqrt((sq[:1, :1] + sq_in[:1, :1]) / entries + 1e-06)
        rate = learn_rate * scale

    def products(slot):
        f = f_all[slot]
        return (jnp.dot(f[:, :rank], u_half[:, :q_cols], preferred_element_type=jnp.float32),
                jnp.dot(f[:, rank:], u_half[:, q_cols:], preferred_element_type=jnp.float32))

    def renew(slot, got_q, got_v):
        at = pl.ds(pl.multiple_of(slot * deep, 16), deep)
        copy_q[at, :] = (w_all[slot, :, :q_cols].astype(jnp.float32) - rate * got_q).astype(jnp.bfloat16)
        copy_v[at, :] = (w_all[slot, :, q_cols:].astype(jnp.float32) - rate * got_v).astype(jnp.bfloat16)

    with scope("own"):
        got_q, got_v = products(p.me)
        renew(p.me, got_q, got_v)
        step_q[...] = scale * got_q
        step_v[...] = scale * got_v
        new_q[...] = qw[...] - rate * got_q
        new_v[...] = vw[...] - rate * got_v
    for i in range(depth):
        for j in range(COLS):
            if i + j > 0:
                with scope(f"mine{j}{i}"):
                    slot = p.at(p.near(i), p.col(j), p.c)
                    renew(slot, *products(slot))
    for i in range(depth):
        for j in range(COLS):
            with scope(f"wc{j}{i}"):
                W.core(j, i)
            with scope(f"theirs{j}{i}"):
                slot = p.at(p.near(i), p.col(j), 1 - p.c)
                renew(slot, *products(slot))
    with scope("drain"):
        m.drain()


def exchange(*args):
    n = lax.axis_size("fs")
    depth = n // (COLS * CORES)
    rows, q_cols = args[7].shape
    v_cols = args[9].shape[1]
    cols = q_cols + v_cols
    rank, deep = rows * n, args[3].shape[0]
    any_, vmem = pl.BlockSpec(memory_space=pl.ANY), pl.BlockSpec(memory_space=pltpu.VMEM)
    f32, bf16 = jnp.float32, jnp.bfloat16
    dma = pltpu.SemaphoreType.DMA
    part = rank // (CORES * COLS)
    groups = semaphores(depth)
    out = pltpu.VMEM
    done = pl.pallas_call(
        functools.partial(kernel, n, tuple(len(group) for group in groups)),
        out_shape=(
            out((deep, q_cols), f32), out((deep, v_cols), f32), out((deep, q_cols), f32), out((deep, v_cols), f32),
            out((rows, q_cols), f32), out((rows, q_cols), f32), out((rows, v_cols), f32), out((rows, v_cols), f32),
            out((n * deep, q_cols), bf16), out((n * deep, v_cols), bf16),
        ),
        in_specs=[any_] * len(args),
        out_specs=(vmem,) * 10,
        scratch_shapes=[pltpu.VMEM(a.shape, a.dtype) for a in args] + [
            pltpu.VMEM((n, deep, 2 * rank), bf16), pltpu.VMEM((n, deep, cols), bf16), pltpu.VMEM((n, rows, cols), bf16),
            pltpu.VMEM((CORES, COLS, part, cols), f32), pltpu.VMEM((COLS, part, cols), f32),
            pltpu.VMEM((part, cols), WIRE), pltpu.VMEM((part, cols), WIRE), pltpu.VMEM((depth, rows, cols), WIRE),
            pltpu.VMEM((depth, rows, cols), WIRE), pltpu.VMEM((depth, rows, cols), f32),
            pltpu.VMEM((rank, cols), f32), pltpu.VMEM((rank, cols), bf16),
            pltpu.VMEM((8, 128), f32), pltpu.VMEM((8, 128), f32),
            pltpu.VMEM((rank, q_cols), f32), pltpu.VMEM((rank, v_cols), f32),
            dma((len(args),)), dma((4,)), dma((depth,)), dma((depth,)), dma((2,)),
        ] + sum(groups, []),
        compiler_params=pltpu.CompilerParams(
            collective_id=0, has_side_effects=True, vmem_limit_bytes=50 * 1024 * 1024),
    )(*args)
    return write_out(done)


def write_kernel(*refs):
    sems, count = refs[-1], len(refs) // 2
    copies = [
        pltpu.make_async_copy(src, dst, sems.at[i]) for i, (src, dst) in enumerate(zip(refs[:count], refs[count:-1]))]
    for copy in copies:
        copy.start()
    for copy in copies:
        copy.wait()


def write_out(arrays):
    count = len(arrays)
    any_ = pl.BlockSpec(memory_space=pl.ANY)
    arrays = [pltpu.with_memory_space_constraint(a, pltpu.VMEM) for a in arrays]
    return pl.pallas_call(
        write_kernel,
        out_shape=tuple(pltpu.HBM(a.shape, a.dtype) for a in arrays),
        in_specs=[any_] * count,
        out_specs=(any_,) * count,
        scratch_shapes=[pltpu.SemaphoreType.DMA((count,))],
        compiler_params=pltpu.CompilerParams(has_side_effects=True, vmem_limit_bytes=1024 * 1024),
    )(*arrays)


def by_collectives(
    inputs, query_cot, value_cot, query_factor, value_factor, query_weight, value_weight,
    query_first, query_second, value_first, value_second,
):
    f_own = jnp.concatenate([query_factor, value_factor], axis=1)
    w_own = jnp.concatenate([query_weight, value_weight], axis=1).astype(jnp.bfloat16)
    q_cols = query_cot.shape[1]
    n, rank = lax.axis_size("fs"), f_own.shape[1] // 2
    entries = rank * (q_cols + value_cot.shape[1]) * lax.axis_size("tp")
    f_all = lax.all_gather(f_own, "fs", axis=0)
    w_all = lax.all_gather(w_own, "fs", axis=0)
    proj = jnp.dot(inputs, f_all.reshape(-1, 2 * rank), preferred_element_type=jnp.float32).astype(jnp.bfloat16)
    over = (((0,), (0,)), ((), ()))
    term_q = lax.dot_general(proj[:, :rank], query_cot, over, preferred_element_type=jnp.float32)
    term_v = lax.dot_general(proj[:, rank:], value_cot, over, preferred_element_type=jnp.float32)
    own = lax.psum_scatter(jnp.concatenate([term_q, term_v], axis=1), "fs", scatter_dimension=0, tiled=True)
    first_q, second_q, unit_q = moments(query_first, query_second, own[:, :q_cols])
    first_v, second_v, unit_v = moments(value_first, value_second, own[:, q_cols:])
    total = lax.psum(jnp.sum(unit_q * unit_q) + jnp.sum(unit_v * unit_v), ("fs", "tp"))
    scale = lax.rsqrt(total / entries + 1e-06)
    mine = (scale * jnp.concatenate([unit_q, unit_v], axis=1)).astype(jnp.bfloat16)
    bits = lax.all_gather(mine, "fs", axis=0, tiled=True)
    f_full = f_all.reshape(-1, 2 * rank)
    w_full = w_all.reshape(-1, w_own.shape[1])
    bits_q, bits_v = bits[:, :q_cols], bits[:, q_cols:]
    f32 = jnp.float32
    step_q = jnp.dot(query_factor, bits_q, preferred_element_type=f32)
    step_v = jnp.dot(value_factor, bits_v, preferred_element_type=f32)
    new_q = query_weight - learn_rate * step_q
    new_v = value_weight - learn_rate * step_v
    all_q = jnp.dot(f_full[:, :rank], bits_q, preferred_element_type=f32)
    all_v = jnp.dot(f_full[:, rank:], bits_v, preferred_element_type=f32)
    copy_q = (w_full[:, :q_cols].astype(f32) - learn_rate * all_q).astype(jnp.bfloat16)
    copy_v = (w_full[:, q_cols:].astype(f32) - learn_rate * all_v).astype(jnp.bfloat16)
    return (step_q, step_v, new_q, new_v, first_q, second_q, first_v, second_v, copy_q, copy_v)


def on_device(*args):
    n = lax.axis_size("fs")
    inputs, query_cot, value_cot, query_factor = args[:4]
    rank, q_cols, v_cols = query_factor.shape[1], query_cot.shape[1], value_cot.shape[1]
    whole = (
        n == DEPTH * COLS * CORES and lax.axis_size("tp") == TPS and q_cols % 128 == 0
        and v_cols % 128 == 0 and (2 * rank) % 128 == 0 and inputs.shape[1] % 128 == 0
        and inputs.shape[0] % 256 == 0 and query_factor.shape[0] % 32 == 0 and rank % 64 == 0
    )
    return (exchange if whole else by_collectives)(*args)


def solution(mesh):
    row, both = P("fs", None), P("fs", "tp")
    in_specs = (row, both, both, row, row) + (both,) * 6
    out_specs = (both,) * 8 + (P(None, "tp"),) * 2
    return jax.shard_map(on_device, mesh=mesh, in_specs=in_specs, out_specs=out_specs, check_vma=False)
```
